32 devices in a mesh: sp: 16 (over z, y, x), tp: 2 (over core).
Axes of the slice: x: 2, y: 2, z: 4, core: 2. Of those that a mesh axis runs over, the one named last changes fastest.
Arguments:
- pool_input: bfloat16 [4096, 1024], P('sp', 'tp'), may hold values from -6 to 6
- residual: bfloat16 [4096, 2048], P(('sp', 'tp')), may hold values from -6 to 6
- pool_weight: bfloat16 [4, 256, 256], replicated, may hold values from -0.375 to 0.375
- pool_gain: float32 [1024], replicated, may hold values from 0.1 to 1.9
- out_weight: bfloat16 [1024, 2048], replicated, may hold values from -0.1875 to 0.1875
- norm_gain: float32 [2048], replicated, may hold values from 0.1 to 1.9
- routes: int32 [4096, 4], P(('sp', 'tp')), may hold values from 0 to 15, all different within a row; in each aligned block of 128 rows (0 to 127, 128 to 255, ...) at most 64 rows name the same one
- route_scores: float32 [4096, 4], P(('sp', 'tp')), may hold values from -1 to 1
- gate_weight: bfloat16 [16, 2048, 2048], P('sp', None, 'tp'), may hold values from -0.375 to 0.375
- up_weight: bfloat16 [16, 2048, 2048], P('sp', None, 'tp'), may hold values from -0.375 to 0.375
- down_weight: bfloat16 [16, 2048, 2048], P('sp', 'tp'), may hold values from -0.0234375 to 0.0234375
Outputs:
- layer_out: bfloat16 [4096, 2048], P(('sp', 'tp'))
The draws below stay inside these ranges and needn't reach their ends.
Inputs may be any that keep to these rules, and one draw needn't show every extreme that they name: `routes`: each row names 4 different experts; among the rows of one device no expert is named more than 64 times, a bound that some block reaches.
All inputs are finite; a program needn't handle non-finite values.
Results may differ from the reference program's by a relative error of at most 0.012.
Values may be sent and summed in bfloat16 or wider, within the bound.
A program may use at most 128 MiB of HBM per device.

```python
import math
import jax
import jax.numpy as jnp
import numpy as np
from jax import lax

D = 2048
GROUPS = 4
GROUP_DIM = 256
FF = 2048
TOPK = 4
TOK_DEV = 256
PW = 1024
EXPERTS = 16
TOKENS = 4096
CAP = 64
N_TP = 2


def steps_of(own_key, shape, cuts, least, high):
    gain = 1.0
    for position, parts in cuts:
        draws = jax.random.uniform(jax.random.fold_in(jax.random.fold_in(own_key, 6), position), (parts,), jnp.float32, least / len(cuts), high / len(cuts))
        gain = gain * jnp.repeat(jnp.exp(draws), shape[position] // parts).reshape((-1,) + (1,) * (len(shape) - 1 - position))
    return gain


def shared_out(own_key, own, number, rows, amount, top, bound, lean):
    sequence = jax.random.permutation(own_key, amount)
    heavy_load, ordinary = shares(amount, rows * top, bound, lean, True), shares(amount, rows * top, bound, lean, False)
    places = jnp.arange(amount)

    def named(sizes, rotation):
        used = int((sizes > 0).sum())
        fixed = max(1, used // 4)
        passed = fixed + (places - fixed + rotation * (used - fixed)) % max(1, amount - fixed)
        return jnp.zeros((amount,), jnp.int32).at[sequence[jnp.where(places < fixed, places, passed)]].set(jnp.asarray(sizes, jnp.int32))

    sizes = jnp.where(number % 4 == 0, named(heavy_load, number // 4), named(ordinary, number - number // 4 - 1))
    mixed = jax.random.permutation(jax.random.fold_in(own, 3), amount)
    giver, receiver = mixed[0:amount // 2 * 2:2], mixed[1:amount // 2 * 2:2]
    room = jnp.minimum(sizes[giver] - 1, bound - sizes[receiver]) // 2
    room = jnp.where((giver == sequence[0]) | (receiver == sequence[0]) | (sizes[receiver] == 0), 0, jnp.maximum(room, 0))
    passed = jax.random.randint(jax.random.fold_in(own, 4), (amount // 2,), 0, 1 << 20) % (room + 1)
    sizes = sizes.at[giver].add(-passed).at[receiver].add(passed)
    members = jnp.searchsorted(jnp.cumsum(sizes), jnp.arange(rows * top), side="right").astype(jnp.int32)
    grid = members.reshape(top, rows).T
    grid = grid[jax.random.permutation(jax.random.fold_in(own, 1), rows)]
    rotation = jax.random.randint(jax.random.fold_in(own, 2), (rows, 1), 0, top)
    return jnp.take_along_axis(grid, (jnp.arange(top)[None, :] + rotation) % top, axis=1)


def shares(amount, total, bound, lean, full):
    loads = [(1 << 20) // math.isqrt(standing ** lean) + 1 for standing in range(1, amount + 1)]
    largest = bound if full else min(bound, max(-(-total // amount), total * loads[0] // sum(loads)))
    least = 1 if total - largest >= amount - 1 else 0
    given, rest = [largest] + [least] * (amount - 1), total - largest - least * (amount - 1)
    while rest > 0:
        candidates = [i for i in range(1, amount) if given[i] < largest] or [i for i in range(1, amount) if given[i] < bound]
        mass, left = sum([loads[i] for i in candidates]), rest
        for i in candidates:
            extra = min(bound - given[i], max(1, left * loads[i] // mass), rest)
            given[i] = given[i] + extra
            rest = rest - extra
    return np.array(given)


def bell_draw(rng, dims, spread, reach, cuts=(), dtype=jnp.bfloat16):
    factor_of = steps_of(rng, dims, cuts, -0.22, 0.18) if cuts else 1.0
    drawn = jax.random.normal(rng, dims, jnp.float32) * spread * factor_of
    return jnp.minimum(jnp.maximum(drawn, -reach), reach).astype(dtype)


def setup_inputs(seed: int = 0) -> dict:
    splits = jax.random.split(jax.random.key(seed), 12)
    pool_input = bell_draw(splits[0], (TOKENS, PW), 1.0, 6.0, ((0, 16), (1, 2)))
    residual = bell_draw(splits[1], (TOKENS, D), 1.0, 6.0, ((0, 32),))
    pool_weight = bell_draw(splits[2], (GROUPS, GROUP_DIM, GROUP_DIM), GROUP_DIM ** -0.5, 0.375)
    pool_gain = jnp.clip(1.0 + 0.18 * jax.random.normal(splits[3], (PW,), jnp.float32), 0.1, 1.9)
    out_weight = bell_draw(splits[4], (PW, D), PW ** -0.5, 0.1875)
    norm_gain = jnp.clip(1.0 + 0.18 * jax.random.normal(splits[5], (D,), jnp.float32), 0.1, 1.9)
    routes_keys = jax.random.split(jax.random.fold_in(splits[6], 1), TOKENS // (TOK_DEV // N_TP))
    routes_turns = jax.random.permutation(jax.random.fold_in(splits[6], 3), TOKENS // (TOK_DEV // N_TP))
    routes = jax.vmap(lambda own, number: shared_out(jax.random.fold_in(splits[6], 2), own, number, TOK_DEV // N_TP, EXPERTS, TOPK, CAP, 1))(routes_keys, routes_turns).reshape((TOKENS, TOPK))
    route_scores = bell_draw(splits[7], (TOKENS, TOPK), 0.4, 1.0, ((0, 32),), jnp.float32)
    gate_weight = bell_draw(splits[8], (EXPERTS, D, FF), (D // 9) ** -0.5, 0.375, ((0, 16), (2, 2)))
    up_weight = bell_draw(splits[9], (EXPERTS, D, FF), (D // 9) ** -0.5, 0.375, ((0, 16), (2, 2)))
    down_weight = bell_draw(splits[10], (EXPERTS, FF, D), (FF * 36) ** -0.5, 0.0234375, ((0, 16), (1, 2)))
    return {"pool_input": pool_input, "residual": residual, "pool_weight": pool_weight, "pool_gain": pool_gain, "out_weight": out_weight, "norm_gain": norm_gain, "routes": routes, "route_scores": route_scores, "gate_weight": gate_weight, "up_weight": up_weight, "down_weight": down_weight}


def expert_rows(rows, gate_matrix, up_matrix, down_matrix):
    gate_pre = jnp.dot(rows, gate_matrix, preferred_element_type=jnp.float32)
    up_pre = jnp.dot(rows, up_matrix, preferred_element_type=jnp.float32)
    clipped_gate = jnp.minimum(gate_pre, 7.0)
    clipped_up = jnp.clip(up_pre, -7.0, 7.0)
    activated = ((clipped_up + 1.0) * (clipped_gate * jax.nn.sigmoid(1.702 * clipped_gate))).astype(jnp.bfloat16)
    middle_unit = FF // 2
    first_half = jnp.dot(activated[:, :middle_unit], down_matrix[:middle_unit], preferred_element_type=jnp.float32).astype(jnp.bfloat16)
    second_half = jnp.dot(activated[:, middle_unit:], down_matrix[middle_unit:], preferred_element_type=jnp.float32).astype(jnp.bfloat16)
    first_half = lax.optimization_barrier(first_half)
    second_half = lax.optimization_barrier(second_half)
    return (first_half.astype(jnp.float32) + second_half.astype(jnp.float32)).astype(jnp.bfloat16)

def reference(pool_input, residual, pool_weight, pool_gain, out_weight, norm_gain, routes, route_scores, gate_weight, up_weight, down_weight):
    length = pool_input.shape[0]
    values = pool_input.astype(jnp.float32)
    padded = jnp.pad(values, ((16, 0), (0, 0)))
    positions = jnp.arange(length).astype(jnp.float32)
    pieces = []
    for group_index in range(GROUPS):
        window = 2 ** (group_index + 1)
        column = padded[:, group_index * GROUP_DIM:(group_index + 1) * GROUP_DIM]
        total = jnp.zeros((length, GROUP_DIM), jnp.float32)
        for offset in range(window):
            total = total + column[16 - offset:16 - offset + length]
        pieces.append(total / jnp.minimum(positions + 1.0, float(window))[:, None])
    pooled = (jnp.concatenate(pieces, axis=1) - values).astype(jnp.bfloat16)
    grouped = jnp.einsum('tgc,gce->tge', pooled.reshape(length, GROUPS, GROUP_DIM).astype(jnp.float32), pool_weight.astype(jnp.float32))
    mixer_out = (grouped.reshape(length, PW) * pool_gain[None, :]).astype(jnp.bfloat16)
    middle = (residual.astype(jnp.float32) + jnp.dot(mixer_out, out_weight, preferred_element_type=jnp.float32)).astype(jnp.bfloat16)
    middle_wide = middle.astype(jnp.float32)
    normed = (middle_wide * lax.rsqrt(lax.optimization_barrier(jnp.mean(middle_wide * middle_wide, axis=1, keepdims=True)) + 1e-05) * norm_gain[None, :]).astype(jnp.bfloat16)
    weights = jax.nn.softmax(route_scores.astype(jnp.float32), axis=-1)
    block_rows = 256
    count_routes = TOKENS * TOPK
    flat_expert = routes.reshape(-1).astype(jnp.int32)
    order = jnp.argsort(flat_expert, stable=True).astype(jnp.int32)
    sorted_expert = flat_expert[order]
    token_of = (order // TOPK).astype(jnp.int32)
    counts = lax.optimization_barrier(jnp.sum((flat_expert[:, None] == jnp.arange(EXPERTS).astype(jnp.int32)[None, :]).astype(jnp.int32), axis=0))
    starts = (jnp.cumsum(counts) - counts).astype(jnp.int32)
    padded_counts = ((counts + block_rows - 1) // block_rows * block_rows).astype(jnp.int32)
    ends = jnp.cumsum(padded_counts).astype(jnp.int32)
    begins = (ends - padded_counts).astype(jnp.int32)
    destination = (begins[sorted_expert] + jnp.arange(count_routes).astype(jnp.int32) - starts[sorted_expert]).astype(jnp.int32)
    blocks = -(-count_routes // block_rows) + EXPERTS
    slot_token = jnp.zeros((blocks * block_rows,), jnp.int32).at[destination].set(token_of)
    block_expert = jnp.minimum(jnp.searchsorted(ends, (jnp.arange(blocks) * block_rows).astype(jnp.int32), side='right'), EXPERTS - 1).astype(jnp.int32)

    def expert_block(operands):
        tokens_block, expert_id = operands
        return expert_rows(normed[tokens_block], gate_weight[expert_id], up_weight[expert_id], down_weight[expert_id])
    outputs = lax.map(expert_block, (slot_token.reshape(blocks, block_rows), block_expert)).reshape(blocks * block_rows, D)
    route_slot = jnp.zeros((count_routes,), jnp.int32).at[order].set(destination)
    route_rows = outputs[route_slot].astype(jnp.float32).reshape(TOKENS, TOPK, D)
    mixture = lax.optimization_barrier(jnp.sum(route_rows * weights[:, :, None], axis=1))
    return (middle_wide + mixture).astype(jnp.bfloat16)
```

```python
import functools

import jax
import jax.numpy as jnp
from jax import lax
from jax.experimental import pallas as pl
from jax.experimental.pallas import tpu as pltpu
from jax.sharding import PartitionSpec as P

MESH = pl.DeviceIdType.MESH
F32, BF16 = jnp.float32, jnp.bfloat16


def xor(index, mask):
    out, bit = index, 1
    while bit <= mask:
        if mask // bit % 2:
            out = out + bit - 2 * bit * (index // bit % 2)
        bit *= 2
    return out


def layer_kernel(
    planes,
    ways,
    cap,
    normed_ref,
    meta_ref,
    middle_ref,
    gate_hbm,
    up_hbm,
    down_hbm,
    out_ref,
    gate_w,
    up_w,
    down_w,
    tok,
    metas,
    snd,
    rows,
    act,
    part,
    part_in,
    back,
    mix_in,
    acc,
    w_sem,
    z_sem,
    m_sem,
    a_send,
    a_recv,
    f_sem,
    p_sem,
    r_send,
    r_recv,
    x_sem,
):
    sp, core = lax.axis_index("sp"), lax.axis_index("tp")
    z, p = sp // ways, sp % ways
    tokens, width = normed_ref.shape
    hidden = gate_w.shape[1]
    experts = meta_ref.shape[0] // 2

    def z_peer(k):
        return (xor(z, k) * ways + p, core)

    def p_peer(q):
        return (z * ways + xor(p, q), core)

    sibling = (sp, 1 - core)

    barrier = pltpu.get_barrier_semaphore()
    for k in range(1, planes):
        pl.semaphore_signal(barrier, inc=1, device_id=z_peer(k), device_id_type=MESH)
    for q in range(1, ways):
        pl.semaphore_signal(barrier, inc=1, device_id=p_peer(q), device_id_type=MESH)
    pl.semaphore_signal(barrier, inc=1, device_id=sibling, device_id_type=MESH)
    pl.semaphore_wait(barrier, planes + ways - 1)

    def remote(src, dst, send, recv, device):
        return pltpu.make_async_remote_copy(
            src_ref=src,
            dst_ref=dst,
            send_sem=send,
            recv_sem=recv,
            device_id=device,
            device_id_type=MESH,
        )

    z_copies, m_copies = {}, {}
    for k in range(1, planes):
        m_copies[k] = remote(meta_ref, metas.at[k], m_sem.at[0, k], m_sem.at[1, k], z_peer(k))
        m_copies[k].start()
    for k in range(1, planes):
        z_copies[k] = remote(normed_ref, tok.at[k], z_sem.at[0, k], z_sem.at[1, k], z_peer(k))
        z_copies[k].start()
    loads = [
        pltpu.make_async_copy(src, dst, w_sem.at[i])
        for i, (src, dst) in enumerate(((gate_hbm, gate_w), (up_hbm, up_w), (down_hbm, down_w)))
    ]
    for load in loads:
        load.start()

    slot_of = lax.broadcasted_iota(jnp.int32, (cap, tokens), 0).astype(F32)

    def meta_row(k, row):
        if k == 0:
            return meta_ref[pl.ds(row, 1), :]
        return metas[k, pl.ds(row, 1), :]

    a_copies, r_copies, f_copies, p_copies, x_copies = {}, {}, {}, {}, {}

    def pick(k):
        if k:
            m_copies[k].wait_recv()
            z_copies[k].wait_recv()
        source = normed_ref if k == 0 else tok.at[k]
        order = list(range(1, ways)) + [0]
        for q in order:
            expert = z * ways + xor(p, q)
            choose = jnp.where(meta_row(k, expert) == slot_of, 1.0, 0.0).astype(BF16)
            chosen = jnp.dot(choose, source[...], preferred_element_type=F32).astype(BF16)
            if q == 0:
                rows[k, core, 0] = chosen
            else:
                snd[k, q] = chosen
                a_copies[k, q] = remote(
                    snd.at[k, q], rows.at[k, core, q], a_send.at[k, q], a_recv.at[k, q], p_peer(q)
                )
                a_copies[k, q].start()

    def forward(k):
        for q in range(1, ways):
            a_copies[k, q].wait_recv()
        f_copies[k] = remote(
            rows.at[k, core], rows.at[k, core], f_sem.at[0, k], f_sem.at[1, k], sibling
        )
        f_copies[k].start()

    half = ways * cap
    step_f = min(hidden, 256)
    step_d = min(width, 256)

    def expert(k):
        f_copies[k].wait_recv()

        def gated(i, carry):
            cols = pl.ds(pl.multiple_of(i * step_f, step_f), step_f)
            these = rows[k].reshape(2 * half, width)
            gate_pre = jnp.dot(these, gate_w[:, cols], preferred_element_type=F32)
            up_pre = jnp.dot(these, up_w[:, cols], preferred_element_type=F32)
            a = jnp.minimum(gate_pre, 7.0)
            b = jnp.clip(up_pre, -7.0, 7.0) + 1.0
            act[:, cols] = (b * (a * jax.nn.sigmoid(1.702 * a))).astype(BF16)
            return carry

        lax.fori_loop(0, hidden // step_f, gated, 0)

        def down(i, carry):
            cols = pl.ds(pl.multiple_of(i * step_d, step_d), step_d)
            value = jnp.dot(act[...], down_w[:, cols], preferred_element_type=F32).astype(BF16)
            part[k, :, :, cols] = value.reshape(2, half, step_d)
            return carry

        if k == 0:
            loads[2].wait()
        lax.fori_loop(0, width // step_d, down, 0)
        p_copies[k] = remote(
            part.at[k, 1 - core], part_in.at[k], p_sem.at[0, k], p_sem.at[1, k], sibling
        )
        p_copies[k].start()

    def give_back(k):
        p_copies[k].wait_recv()
        for q in list(range(1, ways)) + [0]:
            here = pl.ds(q * cap, cap)
            total = (part[k, core, here, :].astype(F32) + part_in[k, here, :].astype(F32)).astype(
                BF16
            )
            if q == 0:
                back[k, 0] = total
            else:
                a_copies[k, q].wait_send()
                snd[k, q] = total
                r_copies[k, q] = remote(
                    snd.at[k, q], back.at[k, q], r_send.at[k, q], r_recv.at[k, q], p_peer(q)
                )
                r_copies[k, q].start()

    def combine(k):
        blocks = []
        for q in range(ways):
            if q:
                r_copies[k, q].wait_recv()
            index = z * ways + xor(p, q)
            blocks.append(
                jnp.where(meta_row(k, index) == slot_of, meta_row(k, index + experts), 0.0)
            )
        mixer = jnp.transpose(jnp.concatenate(blocks, axis=0))
        high = mixer.astype(BF16)
        low = (mixer - high.astype(F32)).astype(BF16)

        def mixed(i, carry):
            cols = pl.ds(pl.multiple_of(i * step_d, step_d), step_d)
            values = back[k, :, :, cols].reshape(half, step_d)
            total = jnp.dot(high, values, preferred_element_type=F32) + jnp.dot(
                low, values, preferred_element_type=F32
            )
            if k == 0:
                acc[:, cols] = total
            else:
                tok[k, :, cols] = total.astype(BF16)
            return carry

        lax.fori_loop(0, width // step_d, mixed, 0)
        if k:
            x_copies[k] = remote(
                tok.at[k], mix_in.at[k], x_sem.at[0, k], x_sem.at[1, k], z_peer(k)
            )
            x_copies[k].start()

    pick(0)
    loads[0].wait()
    loads[1].wait()
    for k in range(planes):
        if k + 1 < planes:
            forward(k)
            pick(k + 1)
        else:
            forward(k)
        expert(k)
        if k:
            combine(k - 1)
        give_back(k)
    combine(planes - 1)

    for k in range(1, planes):
        x_copies[k].wait_recv()
        acc[...] += mix_in[k].astype(F32)
    out_ref[...] = (middle_ref[...].astype(F32) + acc[...]).astype(out_ref.dtype)

    for k in range(1, planes):
        m_copies[k].wait_send()
        z_copies[k].wait_send()
        x_copies[k].wait_send()
    for k in range(planes):
        f_copies[k].wait_send()
        p_copies[k].wait_send()
        for q in range(1, ways):
            r_copies[k, q].wait_send()


def experts_layer(normed, meta, middle, gate, up, down, cap):
    tokens, width = normed.shape
    hidden = gate.shape[1]
    size = lax.axis_size("sp")
    planes = 1 << ((size.bit_length() - 1) // 2)
    ways = size // planes
    vmem = pl.BlockSpec(memory_space=pltpu.VMEM)
    hbm = pl.BlockSpec(memory_space=pltpu.HBM)
    dma = pltpu.SemaphoreType.DMA
    return pl.pallas_call(
        functools.partial(layer_kernel, planes, ways, cap),
        out_shape=jax.ShapeDtypeStruct((tokens, width), BF16),
        in_specs=[vmem, vmem, vmem, hbm, hbm, hbm],
        out_specs=vmem,
        scratch_shapes=[
            pltpu.VMEM((width, hidden), BF16),
            pltpu.VMEM((width, hidden), BF16),
            pltpu.VMEM((hidden, width), BF16),
            pltpu.VMEM((planes, tokens, width), BF16),
            pltpu.VMEM((planes,) + meta.shape, F32),
            pltpu.VMEM((planes, ways, cap, width), BF16),
            pltpu.VMEM((planes, 2, ways, cap, width), BF16),
            pltpu.VMEM((2 * ways * cap, hidden), BF16),
            pltpu.VMEM((planes, 2, ways * cap, width), BF16),
            pltpu.VMEM((planes, ways * cap, width), BF16),
            pltpu.VMEM((planes, ways, cap, width), BF16),
            pltpu.VMEM((planes, tokens, width), BF16),
            pltpu.VMEM((tokens, width), F32),
            dma((3,)),
            dma((2, planes)),
            dma((2, planes)),
            dma((planes, ways)),
            dma((planes, ways)),
            dma((2, planes)),
            dma((2, planes)),
            dma((planes, ways)),
            dma((planes, ways)),
            dma((2, planes)),
        ],
        compiler_params=pltpu.CompilerParams(
            collective_id=0, has_side_effects=True, vmem_limit_bytes=67043328 - (2 << 20)
        ),
    )(normed, meta, middle, gate, up, down)


def shards(
    pool_input,
    residual,
    pool_weight,
    pool_gain,
    out_weight,
    norm_gain,
    routes,
    route_scores,
    gate_weight,
    up_weight,
    down_weight,
):
    tokens_here, width_here = pool_input.shape
    cores = lax.axis_size("tp")
    groups, group_dim = pool_weight.shape[:2]
    core = lax.axis_index("tp")
    count = tokens_here // cores
    reach = 1 << groups
    devices = lax.axis_size("sp")
    previous = lax.ppermute(
        pool_input[tokens_here - reach :], "sp", [(i, i + 1) for i in range(devices - 1)]
    )
    extended = jnp.concatenate([previous, pool_input], axis=0)
    theirs = lax.ppermute(
        lax.dynamic_slice_in_dim(extended, (1 - core) * count, count + reach, 0),
        "tp",
        [(0, 1), (1, 0)],
    )
    mine = lax.dynamic_slice_in_dim(extended, core * count, count + reach, 0)
    first = core == 0
    halves = (jnp.where(first, mine, theirs), jnp.where(first, theirs, mine))
    values = jnp.concatenate(halves, axis=1).astype(F32)
    positions = (
        lax.axis_index("sp") * tokens_here + core * count + jnp.arange(count)
    ).astype(F32)[:, None]
    pieces = []
    for group in range(groups):
        total = values[:, group * group_dim : (group + 1) * group_dim]
        here = total[reach:]
        for level in range(group + 1):
            shift = 1 << level
            total = total[shift:] + total[:-shift]
        window = 2 << group
        total = total[total.shape[0] - count :]
        pooled = (total / jnp.minimum(positions + 1.0, float(window)) - here).astype(BF16)
        pieces.append(jnp.dot(pooled, pool_weight[group], preferred_element_type=F32))
    mixer_out = (jnp.concatenate(pieces, axis=1) * pool_gain[None, :]).astype(BF16)
    projected = jnp.dot(mixer_out, out_weight, preferred_element_type=F32)
    middle = (residual.astype(F32) + projected).astype(BF16)
    wide = middle.astype(F32)
    normed = (
        wide
        * lax.rsqrt(jnp.mean(wide * wide, axis=1, keepdims=True) + 1e-05)
        * norm_gain[None, :]
    ).astype(BF16)
    weights = jax.nn.softmax(route_scores, axis=-1)
    row_count, top_count = routes.shape
    experts_total = gate_weight.shape[0] * devices
    cap = row_count * top_count * cores // experts_total
    named = routes.T[:, None, :] == jnp.arange(experts_total)[None, :, None]
    hits = jnp.any(named, axis=0)
    share = jnp.sum(jnp.where(named, weights.T[:, None, :], 0.0), axis=0)
    before = (jnp.arange(row_count)[:, None] < jnp.arange(row_count)[None, :]).astype(BF16)
    rank = jnp.dot(hits.astype(BF16), before, preferred_element_type=F32)
    meta = jnp.concatenate([jnp.where(hits, rank, -1.0), share], axis=0)
    return experts_layer(
        normed, meta, middle, gate_weight[0], up_weight[0], down_weight[0], cap
    )


def solution(mesh):
    return jax.shard_map(
        shards,
        mesh=mesh,
        in_specs=(
            P("sp", "tp"),
            P(("sp", "tp"), None),
            P(),
            P(),
            P(),
            P(),
            P(("sp", "tp"), None),
            P(("sp", "tp"), None),
            P("sp", None, "tp"),
            P("sp", None, "tp"),
            P("sp", "tp", None),
        ),
        out_specs=P(("sp", "tp"), None),
        check_vma=False,
    )
```

```python
import functools

import jax
import jax.numpy as jnp
from jax import lax
from jax.experimental import pallas as pl
from jax.experimental.pallas import tpu as pltpu
from jax.sharding import PartitionSpec as P

MESH = pl.DeviceIdType.MESH
F32, BF16 = jnp.float32, jnp.bfloat16


def xor(index, mask):
    out, bit = index, 1
    while bit <= mask:
        if mask // bit % 2:
            out = out + bit - 2 * bit * (index // bit % 2)
        bit *= 2
    return out


def layer_kernel(
    planes,
    ways,
    cap,
    normed_ref,
    meta_ref,
    middle_ref,
    gate_hbm,
    up_hbm,
    down_hbm,
    out_ref,
    gate_w,
    up_w,
    down_w,
    tok,
    metas,
    snd,
    rows,
    act,
    part,
    part_in,
    back,
    mix_in,
    acc,
    w_sem,
    z_sem,
    m_sem,
    a_send,
    a_recv,
    f_sem,
    p_sem,
    r_send,
    r_recv,
    x_sem,
):
    sp, core = lax.axis_index("sp"), lax.axis_index("tp")
    z, p = sp // ways, sp % ways
    tokens, width = normed_ref.shape
    hidden = gate_w.shape[1]
    experts = meta_ref.shape[0] // 2

    def z_peer(k):
        return (xor(z, k) * ways + p, core)

    def p_peer(q):
        return (z * ways + xor(p, q), core)

    sibling = (sp, 1 - core)

    barrier = pltpu.get_barrier_semaphore()
    for k in range(1, planes):
        pl.semaphore_signal(barrier, inc=1, device_id=z_peer(k), device_id_type=MESH)
    for q in range(1, ways):
        pl.semaphore_signal(barrier, inc=1, device_id=p_peer(q), device_id_type=MESH)
    pl.semaphore_signal(barrier, inc=1, device_id=sibling, device_id_type=MESH)
    pl.semaphore_wait(barrier, planes + ways - 1)

    def remote(src, dst, send, recv, device):
        return pltpu.make_async_remote_copy(
            src_ref=src,
            dst_ref=dst,
            send_sem=send,
            recv_sem=recv,
            device_id=device,
            device_id_type=MESH,
        )

    z_copies, m_copies = {}, {}
    for k in range(1, planes):
        m_copies[k] = remote(meta_ref, metas.at[k], m_sem.at[0, k], m_sem.at[1, k], z_peer(k))
        m_copies[k].start()
    order = [0] + list(range(planes - 1, 0, -1))
    relayed = planes >= 4

    def send_own(k):
        z_copies[k] = remote(normed_ref, tok.at[k], z_sem.at[0, k], z_sem.at[1, k], z_peer(k))
        z_copies[k].start()

    for k in order[1:]:
        if not relayed or k > 2:
            send_own(k)
    loads = [
        pltpu.make_async_copy(src, dst, w_sem.at[i])
        for i, (src, dst) in enumerate(((gate_hbm, gate_w), (up_hbm, up_w), (down_hbm, down_w)))
    ]
    for load in loads:
        load.start()

    slot_of = lax.broadcasted_iota(jnp.int32, (cap, tokens), 0).astype(F32)

    def meta_row(k, row):
        if k == 0:
            return meta_ref[pl.ds(row, 1), :]
        return metas[k, pl.ds(row, 1), :]

    a_copies, r_copies, f_copies, p_copies, x_copies = {}, {}, {}, {}, {}

    def pick(k):
        if k:
            m_copies[k].wait_recv()
            z_copies[k].wait_recv()
        if relayed and k == 3:
            z_copies[2] = remote(tok.at[3], tok.at[2], z_sem.at[0, 2], z_sem.at[1, 2], z_peer(1))
            z_copies[2].start()
            send_own(1)
        source = normed_ref if k == 0 else tok.at[k]
        for q in list(range(1, ways)) + [0]:
            expert = z * ways + xor(p, q)
            choose = jnp.where(meta_row(k, expert) == slot_of, 1.0, 0.0).astype(BF16)
            chosen = jnp.dot(choose, source[...], preferred_element_type=F32).astype(BF16)
            if q == 0:
                rows[k, core, 0] = chosen
            else:
                snd[k, q] = chosen
                a_copies[k, q] = remote(
                    snd.at[k, q], rows.at[k, core, q], a_send.at[k, q], a_recv.at[k, q], p_peer(q)
                )
                a_copies[k, q].start()

    def forward(k):
        for q in range(1, ways):
            a_copies[k, q].wait_recv()
        f_copies[k] = remote(
            rows.at[k, core], rows.at[k, core], f_sem.at[0, k], f_sem.at[1, k], sibling
        )
        f_copies[k].start()

    half = ways * cap
    step_f = min(hidden, 256)
    step_d = min(width, 256)

    def expert(k):
        f_copies[k].wait_recv()

        def gated(i, carry):
            cols = pl.ds(pl.multiple_of(i * step_f, step_f), step_f)
            these = rows[k].reshape(2 * half, width)
            gate_pre = jnp.dot(these, gate_w[:, cols], preferred_element_type=F32)
            up_pre = jnp.dot(these, up_w[:, cols], preferred_element_type=F32)
            a = jnp.minimum(gate_pre, 7.0)
            b = jnp.clip(up_pre, -7.0, 7.0) + 1.0
            act[:, cols] = (b * (a * jax.nn.sigmoid(1.702 * a))).astype(BF16)
            return carry

        lax.fori_loop(0, hidden // step_f, gated, 0)

        def down(i, carry):
            cols = pl.ds(pl.multiple_of(i * step_d, step_d), step_d)
            value = jnp.dot(act[...], down_w[:, cols], preferred_element_type=F32).astype(BF16)
            part[k, :, :, cols] = value.reshape(2, half, step_d)
            return carry

        if k == 0:
            loads[2].wait()
        lax.fori_loop(0, width // step_d, down, 0)
        p_copies[k] = remote(
            part.at[k, 1 - core], part_in.at[k], p_sem.at[0, k], p_sem.at[1, k], sibling
        )
        p_copies[k].start()

    def give_back(k):
        p_copies[k].wait_recv()
        for q in list(range(1, ways)) + [0]:
            here = pl.ds(q * cap, cap)
            total = (part[k, core, here, :].astype(F32) + part_in[k, here, :].astype(F32)).astype(
                BF16
            )
            if q == 0:
                back[k, 0] = total
            else:
                a_copies[k, q].wait_send()
                snd[k, q] = total
                r_copies[k, q] = remote(
                    snd.at[k, q], back.at[k, q], r_send.at[k, q], r_recv.at[k, q], p_peer(q)
                )
                r_copies[k, q].start()

    def combine(k):
        if relayed and k == 3:
            z_copies[2].wait_send()
        blocks = []
        for q in range(ways):
            if q:
                r_copies[k, q].wait_recv()
            index = z * ways + xor(p, q)
            blocks.append(
                jnp.where(meta_row(k, index) == slot_of, meta_row(k, index + experts), 0.0)
            )
        mixer = jnp.transpose(jnp.concatenate(blocks, axis=0))
        high = mixer.astype(BF16)
        low = (mixer - high.astype(F32)).astype(BF16)

        def mixed(i, carry):
            cols = pl.ds(pl.multiple_of(i * step_d, step_d), step_d)
            values = back[k, :, :, cols].reshape(half, step_d)
            total = jnp.dot(high, values, preferred_element_type=F32) + jnp.dot(
                low, values, preferred_element_type=F32
            )
            if k == 0:
                acc[:, cols] = total
            else:
                tok[k, :, cols] = total.astype(BF16)
            return carry

        lax.fori_loop(0, width // step_d, mixed, 0)
        if k:
            x_copies[k] = remote(
                tok.at[k], mix_in.at[k], x_sem.at[0, k], x_sem.at[1, k], z_peer(k)
            )
            x_copies[k].start()

    pick(0)
    loads[0].wait()
    loads[1].wait()
    for i, k in enumerate(order):
        forward(k)
        if i + 1 < planes:
            pick(order[i + 1])
        expert(k)
        if i:
            combine(order[i - 1])
        give_back(k)
    combine(order[-1])

    for k in range(1, planes):
        x_copies[k].wait_recv()
        acc[...] += mix_in[k].astype(F32)
    out_ref[...] = (middle_ref[...].astype(F32) + acc[...]).astype(out_ref.dtype)

    for k in range(1, planes):
        m_copies[k].wait_send()
        if not relayed or k != 2:
            z_copies[k].wait_send()
        x_copies[k].wait_send()
    for k in range(planes):
        f_copies[k].wait_send()
        p_copies[k].wait_send()
        for q in range(1, ways):
            r_copies[k, q].wait_send()


def experts_layer(normed, meta, middle, gate, up, down, cap):
    tokens, width = normed.shape
    hidden = gate.shape[1]
    size = lax.axis_size("sp")
    planes = 1 << ((size.bit_length() - 1) // 2)
    ways = size // planes
    vmem = pl.BlockSpec(memory_space=pltpu.VMEM)
    hbm = pl.BlockSpec(memory_space=pltpu.HBM)
    dma = pltpu.SemaphoreType.DMA
    return pl.pallas_call(
        functools.partial(layer_kernel, planes, ways, cap),
        out_shape=jax.ShapeDtypeStruct((tokens, width), BF16),
        in_specs=[vmem, vmem, vmem, hbm, hbm, hbm],
        out_specs=vmem,
        scratch_shapes=[
            pltpu.VMEM((width, hidden), BF16),
            pltpu.VMEM((width, hidden), BF16),
            pltpu.VMEM((hidden, width), BF16),
            pltpu.VMEM((planes, tokens, width), BF16),
            pltpu.VMEM((planes,) + meta.shape, F32),
            pltpu.VMEM((planes, ways, cap, width), BF16),
            pltpu.VMEM((planes, 2, ways, cap, width), BF16),
            pltpu.VMEM((2 * ways * cap, hidden), BF16),
            pltpu.VMEM((planes, 2, ways * cap, width), BF16),
            pltpu.VMEM((planes, ways * cap, width), BF16),
            pltpu.VMEM((planes, ways, cap, width), BF16),
            pltpu.VMEM((planes, tokens, width), BF16),
            pltpu.VMEM((tokens, width), F32),
            dma((3,)),
            dma((2, planes)),
            dma((2, planes)),
            dma((planes, ways)),
            dma((planes, ways)),
            dma((2, planes)),
            dma((2, planes)),
            dma((planes, ways)),
            dma((planes, ways)),
            dma((2, planes)),
        ],
        compiler_params=pltpu.CompilerParams(
            collective_id=0, has_side_effects=True, vmem_limit_bytes=67043328 - (2 << 20)
        ),
    )(normed, meta, middle, gate, up, down)


def shards(
    pool_input,
    residual,
    pool_weight,
    pool_gain,
    out_weight,
    norm_gain,
    routes,
    route_scores,
    gate_weight,
    up_weight,
    down_weight,
):
    tokens_here, width_here = pool_input.shape
    cores = lax.axis_size("tp")
    groups, group_dim = pool_weight.shape[:2]
    core = lax.axis_index("tp")
    count = tokens_here // cores
    reach = 1 << groups
    devices = lax.axis_size("sp")
    previous = lax.ppermute(
        pool_input[tokens_here - reach :], "sp", [(i, i + 1) for i in range(devices - 1)]
    )
    extended = jnp.concatenate([previous, pool_input], axis=0)
    theirs = lax.ppermute(
        lax.dynamic_slice_in_dim(extended, (1 - core) * count, count + reach, 0),
        "tp",
        [(0, 1), (1, 0)],
    )
    mine = lax.dynamic_slice_in_dim(extended, core * count, count + reach, 0)
    first = core == 0
    halves = (jnp.where(first, mine, theirs), jnp.where(first, theirs, mine))
    values = jnp.concatenate(halves, axis=1).astype(F32)
    positions = (
        lax.axis_index("sp") * tokens_here + core * count + jnp.arange(count)
    ).astype(F32)[:, None]
    pieces = []
    for group in range(groups):
        total = values[:, group * group_dim : (group + 1) * group_dim]
        here = total[reach:]
        for level in range(group + 1):
            shift = 1 << level
            total = total[shift:] + total[:-shift]
        window = 2 << group
        total = total[total.shape[0] - count :]
        pooled = (total / jnp.minimum(positions + 1.0, float(window)) - here).astype(BF16)
        pieces.append(jnp.dot(pooled, pool_weight[group], preferred_element_type=F32))
    mixer_out = (jnp.concatenate(pieces, axis=1) * pool_gain[None, :]).astype(BF16)
    projected = jnp.dot(mixer_out, out_weight, preferred_element_type=F32)
    middle = (residual.astype(F32) + projected).astype(BF16)
    wide = middle.astype(F32)
    normed = (
        wide
        * lax.rsqrt(jnp.mean(wide * wide, axis=1, keepdims=True) + 1e-05)
        * norm_gain[None, :]
    ).astype(BF16)
    weights = jax.nn.softmax(route_scores, axis=-1)
    row_count, top_count = routes.shape
    experts_total = gate_weight.shape[0] * devices
    cap = row_count * top_count * cores // experts_total
    named = routes.T[:, None, :] == jnp.arange(experts_total)[None, :, None]
    hits = jnp.any(named, axis=0)
    share = jnp.sum(jnp.where(named, weights.T[:, None, :], 0.0), axis=0)
    before = (jnp.arange(row_count)[:, None] < jnp.arange(row_count)[None, :]).astype(BF16)
    rank = jnp.dot(hits.astype(BF16), before, preferred_element_type=F32)
    meta = jnp.concatenate([jnp.where(hits, rank, -1.0), share], axis=0)
    return experts_layer(
        normed, meta, middle, gate_weight[0], up_weight[0], down_weight[0], cap
    )


def solution(mesh):
    return jax.shard_map(
        shards,
        mesh=mesh,
        in_specs=(
            P("sp", "tp"),
            P(("sp", "tp"), None),
            P(),
            P(),
            P(),
            P(),
            P(("sp", "tp"), None),
            P(("sp", "tp"), None),
            P("sp", None, "tp"),
            P("sp", None, "tp"),
            P("sp", "tp", None),
        ),
        out_specs=P(("sp", "tp"), None),
        check_vma=False,
    )
```
